32 devices in a mesh: kv: 4 (over z), tp: 8 (over y, x, core).
Axes of the slice: x: 2, y: 2, z: 4, core: 2. Of those that a mesh axis runs over, the one named last changes fastest.
Arguments:
- piece_tokens: bfloat16 [512, 2048], P('kv'), may hold values from -6 to 6
- dec_tokens: bfloat16 [8, 2048], P('kv'), may hold values from -6 to 6
- norm_gain: float32 [2048], replicated, may hold values from 0.1 to 1.9
- w_query_nope: bfloat16 [2048, 2048], P(None, 'tp'), may hold values from -0.125 to 0.125
- w_query_rope: bfloat16 [2048, 1024], P(None, 'tp'), may hold values from -0.125 to 0.125
- w_latent: bfloat16 [2048, 512], replicated, may hold values from -0.125 to 0.125
- w_key_rope: bfloat16 [2048, 64], replicated, may hold values from -0.125 to 0.125
- latent_gain: float32 [512], replicated, may hold values from 0.1 to 1.9
- w_key_up: bfloat16 [16, 128, 512], P('tp'), may hold values from -0.5 to 0.5
- w_value_up: bfloat16 [16, 512, 128], P('tp'), may hold values from -3 to 3
- w_out: bfloat16 [2048, 2048], P(None, 'tp'), may hold values from -0.25 to 0.25
- prompt_latent: bfloat16 [2048, 512], P('kv'), may hold values from -210 to 210
- prompt_rope: bfloat16 [2048, 64], P('kv'), may hold values from -6 to 6
- dec_latent: bfloat16 [8, 1024, 512], P('kv'), may hold values from -210 to 210
- dec_rope: bfloat16 [8, 1024, 64], P('kv'), may hold values from -6 to 6
- dec_lengths: int32 [8], P('kv'), may hold values from 1 to 1024, 4096 in all
Outputs:
- piece_out: bfloat16 [512, 2048], P('kv', 'tp')
- dec_out: bfloat16 [8, 2048], P('kv', 'tp')
The draws below stay inside these ranges and needn't reach their ends.
Inputs may be any that keep to these rules, and one draw needn't show every extreme that they name: `dec_lengths`: every decoding sequence has at least one live cache slot, and some sequence has all 1024.
All inputs are finite; a program needn't handle non-finite values. No bound on the sum of `dec_lengths` on one device may be relied on, other than what follows from the above.
Results may differ from the reference program's by a relative error of at most 0.025.
Values may be sent and summed in bfloat16 or wider, within the bound.
No kernel may reach another device: no remote copies, remote signals or barrier semaphores. Data moves between devices by JAX's collectives and lax.ppermute only.
A program may use at most 128 MiB of HBM per device.

```python
import math
import jax
import jax.numpy as jnp
import numpy as np
from jax import lax

D = 2048
HEADS = 16
NOPE = 128
ROPE = 64
VDIM = 128
LATENT = 512
PIECE_DEV = 128
CTX_DEV = 512
DEC_CTX = 1024
PIECE = 512
CTX = 2048
DEC = 8
N_KV = 4


def drawn(key, shape):
    base_key = jax.random.fold_in(key, 0)
    return jnp.clip(jax.random.normal(base_key, shape, jnp.float32), -6.0, 6.0)


def draw_prompt_latent(key, part):
    return drawn(jax.random.fold_in(key, 11), (CTX, LATENT)).astype(jnp.bfloat16)


def draw_dec_latent(key, part):
    return drawn(jax.random.fold_in(key, 12), (DEC, DEC_CTX, LATENT)).astype(jnp.bfloat16)


def block_levels(own_key, dims, shards, least, largest):
    level = 1.0
    for dim, blocks in shards:
        steps = jax.random.uniform(jax.random.fold_in(jax.random.fold_in(own_key, 6), dim), (blocks,), jnp.float32, least / len(shards), largest / len(shards))
        level = level * jnp.repeat(jnp.exp(steps), dims[dim] // blocks).reshape((-1,) + (1,) * (len(dims) - 1 - dim))
    return level


def split_up(amount, total, limit, skew):
    portions = [(1 << 20) // math.isqrt(rank ** skew) + 1 for rank in range(2, amount + 1)]
    surplus, holding = total - limit - (amount - 1), [1] * (amount - 1)
    while surplus > 0:
        free = [i for i in range(amount - 1) if holding[i] < limit]
        pool, remaining = sum([portions[i] for i in free]), surplus
        for i in free:
            more = min(limit - holding[i], max(1, remaining * portions[i] // pool), surplus)
            holding[i] = holding[i] + more
            surplus = surplus - more
    return np.array([limit] + holding)


def ragged_sizes(rng, number_of, total, limit, slope):
    if number_of == 2:
        one = jax.random.randint(rng, (), max(1, total - limit), min(limit, total - 1) + 1)
        return jnp.stack([one, total - one])
    tallies = jnp.asarray(split_up(number_of, total, limit, slope), jnp.int32)
    pairs = (number_of - 1) // 2
    donor, receiver = tallies[1:1 + 2 * pairs:2], tallies[2:2 + 2 * pairs:2]
    slack = jnp.minimum(donor - 1, limit - receiver)
    shifted = jax.random.randint(jax.random.fold_in(rng, 1), (pairs,), 0, 1 << 20) % (slack + 1)
    tallies = tallies.at[1:1 + 2 * pairs:2].set(donor - shifted).at[2:2 + 2 * pairs:2].set(receiver + shifted)
    return tallies[jax.random.permutation(jax.random.fold_in(rng, 2), number_of)]


def bell_draw(key, extent, deviation, reach, cuts=(), held_as=jnp.bfloat16):
    gain = block_levels(key, extent, cuts, -0.22, 0.18) if cuts else 1.0
    values = jax.random.normal(key, extent, jnp.float32) * deviation * gain
    return jnp.minimum(jnp.maximum(values, -reach), reach).astype(held_as)


def setup_inputs(seed: int = 0) -> dict:
    splits = jax.random.split(jax.random.key(seed), 17)
    return {
        "piece_tokens": bell_draw(splits[0], (PIECE, D), 1.0, 6.0, ((0, 4),)),
        "dec_tokens": bell_draw(splits[1], (DEC, D), 1.0, 6.0, ((0, 4),)),
        "norm_gain": jnp.clip(1.0 + 0.18 * jax.random.normal(splits[2], (D,), jnp.float32), 0.1, 1.9),
        "w_query_nope": bell_draw(splits[3], (D, HEADS * NOPE), D ** -0.5, 0.125, ((1, 8),)),
        "w_query_rope": bell_draw(splits[4], (D, HEADS * ROPE), D ** -0.5, 0.125, ((1, 8),)),
        "w_latent": bell_draw(splits[5], (D, LATENT), D ** -0.5, 0.125),
        "w_key_rope": bell_draw(splits[6], (D, ROPE), D ** -0.5, 0.125),
        "latent_gain": jnp.clip(1.0 + 0.18 * jax.random.normal(splits[7], (LATENT,), jnp.float32), 0.1, 1.9),
        "w_key_up": bell_draw(splits[8], (HEADS, NOPE, LATENT), NOPE ** -0.5, 0.5, ((0, 8),)),
        "w_value_up": bell_draw(splits[9], (HEADS, LATENT, VDIM), 4 ** -0.5, 3.0, ((0, 8),)),
        "w_out": bell_draw(splits[10], (HEADS * VDIM, D), (HEADS * VDIM // 4) ** -0.5, 0.25, ((1, 8),)),
        "prompt_latent": draw_prompt_latent(jax.random.fold_in(splits[16], 71), 0),
        "prompt_rope": bell_draw(splits[12], (CTX, ROPE), 1.0, 6.0, ((0, 4),)),
        "dec_latent": draw_dec_latent(jax.random.fold_in(splits[16], 71), 0),
        "dec_rope": bell_draw(splits[14], (DEC, DEC_CTX, ROPE), 1.0, 6.0, ((0, 4),)),
        "dec_lengths": ragged_sizes(splits[15], DEC, DEC * DEC_CTX // 2, DEC_CTX, 2).astype(jnp.int32),
    }


epsilon = 1e-06
rope_base = 10000.0
masked = -1e+30

def normalize(values, gain_vec):
    mean_sq = lax.optimization_barrier(jnp.mean(values * values, axis=-1, keepdims=True))
    return values * lax.rsqrt(mean_sq + epsilon) * gain_vec

def rotate(values, positions):
    half_dim = values.shape[-1] // 2
    frequency = rope_base ** (-jnp.arange(half_dim, dtype=jnp.float32) / half_dim)
    angles = (positions.astype(jnp.float32)[:, None] * frequency[None, :])[:, None, :]
    cosines = jnp.cos(angles)
    sine_values = jnp.sin(angles)
    front_half = values[..., :half_dim]
    back_half = values[..., half_dim:]
    return jnp.concatenate([front_half * cosines - back_half * sine_values, front_half * sine_values + back_half * cosines], axis=-1)

def rounded(values):
    return lax.optimization_barrier(values.astype(jnp.bfloat16)).astype(jnp.float32)

def project(tokens, positions, norm_gain, w_query_nope, w_query_rope, w_latent, w_key_rope, latent_gain):
    row_count = tokens.shape[0]
    rope_dim = w_key_rope.shape[1]
    head_count = w_query_rope.shape[1] // rope_dim
    normed = normalize(tokens.astype(jnp.float32), norm_gain).astype(jnp.bfloat16)
    query_nope = jnp.dot(normed, w_query_nope, preferred_element_type=jnp.float32).astype(jnp.bfloat16)
    query_raw = jnp.dot(normed, w_query_rope, preferred_element_type=jnp.float32).reshape(row_count, head_count, rope_dim)
    query_rot = rotate(query_raw, positions).astype(jnp.bfloat16)
    latent = normalize(jnp.dot(normed, w_latent, preferred_element_type=jnp.float32), latent_gain).astype(jnp.bfloat16)
    key_raw = jnp.dot(normed, w_key_rope, preferred_element_type=jnp.float32)[:, None, :]
    key_rot = rotate(key_raw, positions)[:, 0].astype(jnp.bfloat16)
    return (query_nope, query_rot, latent, key_rot)

def absorb(query_nope, w_key_up):
    head_count, nope_dim, _ = w_key_up.shape
    by_head = query_nope.reshape(query_nope.shape[0], head_count, nope_dim)
    return jnp.einsum('nhd,hdc->nhc', by_head.astype(jnp.float32), w_key_up.astype(jnp.float32)).astype(jnp.bfloat16)

def reference(piece_tokens, dec_tokens, norm_gain, w_query_nope, w_query_rope, w_latent, w_key_rope, latent_gain, w_key_up, w_value_up, w_out, prompt_latent, prompt_rope, dec_latent, dec_rope, dec_lengths):
    score_scale = (NOPE + ROPE) ** (-0.5)
    weights_args = (norm_gain, w_query_nope, w_query_rope, w_latent, w_key_rope, latent_gain)
    piece_pos = CTX + jnp.arange(PIECE, dtype=jnp.int32)
    query_nope, query_rot, new_latent, new_rot = project(piece_tokens, piece_pos, *weights_args)
    query_lat = absorb(query_nope, w_key_up)
    key_count = CTX_DEV + PIECE_DEV
    key_latent = jnp.concatenate([prompt_latent.reshape(N_KV, CTX_DEV, LATENT), new_latent.reshape(N_KV, PIECE_DEV, LATENT)], axis=1)
    key_rot = jnp.concatenate([prompt_rope.reshape(N_KV, CTX_DEV, ROPE), new_rot.reshape(N_KV, PIECE_DEV, ROPE)], axis=1)
    flat_latent = key_latent.reshape(N_KV * key_count, LATENT)
    flat_rot = key_rot.reshape(N_KV * key_count, ROPE)
    column = jnp.arange(N_KV * key_count, dtype=jnp.int32)
    inner_pos = column % key_count
    piece_place = column // key_count * PIECE_DEV + inner_pos - CTX_DEV
    query_place = jnp.arange(PIECE, dtype=jnp.int32)
    visible = (inner_pos[None, :] < CTX_DEV) | (piece_place[None, :] <= query_place[:, None])
    latent_f32 = key_latent.astype(jnp.float32)

    def one_head(head_args):
        head_lat, head_rot, w_value = head_args
        scores = (jnp.dot(head_lat, flat_latent.T, preferred_element_type=jnp.float32) + jnp.dot(head_rot, flat_rot.T, preferred_element_type=jnp.float32)) * score_scale
        scores = jnp.where(visible, scores, masked)
        row_peak = lax.optimization_barrier(jnp.max(scores, axis=1, keepdims=True))
        weights = jnp.exp(scores - row_peak)
        weight_sum = lax.optimization_barrier(jnp.sum(weights, axis=1))
        blocks = rounded(weights).reshape(PIECE, N_KV, key_count)
        mixed_lat = jnp.einsum('qjk,jkc->jqc', blocks, latent_f32).astype(jnp.bfloat16)
        mixed_lat = lax.optimization_barrier(mixed_lat)
        block_parts = rounded(jnp.einsum('jqc,cv->jqv', mixed_lat.astype(jnp.float32), w_value.astype(jnp.float32)))
        summed = lax.optimization_barrier(jnp.sum(block_parts, axis=0))
        return (summed / weight_sum[:, None]).astype(jnp.bfloat16)
    piece_heads = lax.map(one_head, (query_lat.transpose(1, 0, 2), query_rot.transpose(1, 0, 2), w_value_up))
    piece_attn = piece_heads.transpose(1, 0, 2).reshape(PIECE, -1)
    dec_nope, dec_rot, own_lat, own_rot = project(dec_tokens, dec_lengths, *weights_args)
    dec_query = absorb(dec_nope, w_key_up).astype(jnp.float32)
    dec_rotf = dec_rot.astype(jnp.float32)
    cache_lat = dec_latent.astype(jnp.float32)
    cache_scores = (jnp.einsum('bhc,bkc->bhk', dec_query, cache_lat) + jnp.einsum('bhr,bkr->bhk', dec_rotf, dec_rope.astype(jnp.float32))) * score_scale
    live_keys = jnp.arange(dec_latent.shape[1], dtype=jnp.int32)[None, None, :] < dec_lengths[:, None, None]
    cache_scores = jnp.where(live_keys, cache_scores, masked)
    own_scores = (jnp.einsum('bhc,bc->bh', dec_query, own_lat.astype(jnp.float32)) + jnp.einsum('bhr,br->bh', dec_rotf, own_rot.astype(jnp.float32))) * score_scale
    dec_peak = jnp.maximum(lax.optimization_barrier(jnp.max(cache_scores, axis=2)), own_scores)
    cache_w = jnp.exp(cache_scores - dec_peak[:, :, None])
    own_w = jnp.exp(own_scores - dec_peak)
    dec_sum = lax.optimization_barrier(jnp.sum(cache_w, axis=2)) + own_w
    dec_mix = (jnp.einsum('bhk,bkc->bhc', rounded(cache_w), cache_lat) + rounded(own_w)[:, :, None] * own_lat.astype(jnp.float32)[:, None, :]).astype(jnp.bfloat16)
    dec_mix = lax.optimization_barrier(dec_mix)
    dec_value = rounded(jnp.einsum('bhc,hcv->bhv', dec_mix.astype(jnp.float32), w_value_up.astype(jnp.float32)))
    dec_attn = (dec_value / dec_sum[:, :, None]).astype(jnp.bfloat16).reshape(DEC, -1)
    piece_out = jnp.dot(piece_attn, w_out, preferred_element_type=jnp.float32).astype(jnp.bfloat16)
    dec_out = jnp.dot(dec_attn, w_out, preferred_element_type=jnp.float32).astype(jnp.bfloat16)
    return (piece_out, dec_out)
```

```python
import functools

import jax
import jax.numpy as jnp
from jax import lax
from jax.experimental import pallas as pl
from jax.experimental.pallas import tpu as pltpu
from jax.sharding import PartitionSpec as P

epsilon = 1e-06
rope_base = 10000.0
masked = -1e30
f32 = jnp.float32
bf16 = jnp.bfloat16
tail = 16


def mm(a, b):
    return jnp.dot(a, b, preferred_element_type=f32)


def mm_t(a, b):
    return lax.dot_general(a, b, (((1,), (1,)), ((), ())), preferred_element_type=f32)


def normalize(values, gain_row):
    mean_sq = jnp.mean(values * values, axis=-1, keepdims=True)
    return values * lax.rsqrt(mean_sq + epsilon) * gain_row


def tables(positions, rope_dim):
    half = rope_dim // 2
    frequency = rope_base ** (-jnp.arange(half, dtype=f32) / half)
    angles = positions.astype(f32)[:, None] * frequency[None, :]
    c, s = jnp.cos(angles), jnp.sin(angles)
    return jnp.concatenate([c, c, c, c, -s, s, -s, s], axis=1)


def rotate(values, table, half):
    width = values.shape[1]
    lane = lax.broadcasted_iota(jnp.int32, values.shape, 1)
    front = (lane % (2 * half)) < half
    partner = jnp.where(front, pltpu.roll(values, width - half, 1), pltpu.roll(values, half, 1))
    return values * table[:, :width] + partner * table[:, width:]


def query_body(piece_ref, dec_ref, gain_ref, wn_ref, wr_ref, tab_ref, normed_ref, q_ref, *, half):
    rows, dec_rows = piece_ref.shape[0], dec_ref.shape[0]
    gain = gain_ref[...]
    dec = normalize(dec_ref[...].astype(f32), gain)
    dec = jnp.concatenate([dec, jnp.zeros((tail - dec_rows, dec.shape[1]), f32)], axis=0)
    normed_ref[:rows, :] = normalize(piece_ref[...].astype(f32), gain).astype(bf16)
    normed_ref[rows:, :] = dec.astype(bf16)
    normed = normed_ref[...]
    nope_width = wn_ref.shape[1]
    q_ref[:, :nope_width] = mm(normed, wn_ref[...]).astype(bf16)
    raw = mm(normed, wr_ref[...])
    table = tab_ref[...]
    for at in range(0, raw.shape[1], 4 * half):
        part = rotate(raw[:, at : at + 4 * half], table, half)
        q_ref[:, nope_width + at : nope_width + at + 4 * half] = part.astype(bf16)


def latent_body(normed_ref, gain_ref, wl_ref, wk_ref, tab_ref, lat_ref, rot_ref, *, half):
    normed = normed_ref[...]
    lat_ref[...] = normalize(mm(normed, wl_ref[...]), gain_ref[...]).astype(bf16)
    raw = mm(normed, wk_ref[...])
    both = rotate(jnp.concatenate([raw, raw], axis=1), tab_ref[...], half)
    rot_ref[...] = both[:, : 2 * half].astype(bf16)


def stacked_queries(q, wk_ref):
    heads, nope, _ = wk_ref.shape
    rope = (q.shape[1] - heads * nope) // heads
    lat = [mm(q[:, h * nope : (h + 1) * nope], wk_ref[h]).astype(bf16) for h in range(heads)]
    first = heads * nope
    rot = [q[:, first + h * rope : first + (h + 1) * rope] for h in range(heads)]
    return jnp.concatenate(lat, axis=0), jnp.concatenate(rot, axis=0)


def attend_body(
    off_ref, q_ref, pl_ref, pr_ref, nl_ref, nr_ref, wk_ref, wv_ref, out_ref, *, rows, scale
):
    heads, _, vdim = wv_ref.shape
    lat, rot = stacked_queries(q_ref[:rows, :], wk_ref)
    prompt, new = pl_ref[...], nl_ref[:rows, :]
    old = (mm_t(lat, prompt) + mm_t(rot, pr_ref[...])) * scale
    cur = (mm_t(lat, new) + mm_t(rot, nr_ref[:rows, :])) * scale
    row = lax.broadcasted_iota(jnp.int32, cur.shape, 0) % rows
    column = lax.broadcasted_iota(jnp.int32, cur.shape, 1)
    cur = jnp.where(column - row <= off_ref[0], cur, masked)
    peak = jnp.maximum(
        jnp.max(old, axis=1, keepdims=True), jnp.max(cur, axis=1, keepdims=True)
    )
    w_old, w_cur = jnp.exp(old - peak), jnp.exp(cur - peak)
    total = jnp.sum(w_old, axis=1, keepdims=True) + jnp.sum(w_cur, axis=1, keepdims=True)
    mix = (mm(w_old.astype(bf16), prompt) + mm(w_cur.astype(bf16), new)).astype(bf16)
    level = peak + jnp.log(total)
    for h in range(heads):
        span = slice(h * rows, (h + 1) * rows)
        lanes = slice(h * vdim, (h + 1) * vdim)
        value = mm(mix[span], wv_ref[h])
        out_ref[:rows, lanes] = (value / total[span]).astype(bf16)
        flat = jnp.transpose(jnp.broadcast_to(level[span], (rows, 128)))[:tail]
        high = flat.astype(bf16).astype(f32)
        middle = (flat - high).astype(bf16).astype(f32)
        low = flat - high - middle
        line = lax.broadcasted_iota(jnp.int32, flat.shape, 0)
        parts = jnp.where(line == 0, high, jnp.where(line == 1, middle, low))
        out_ref[rows:, lanes] = jnp.where(line < 3, parts, 0.0).astype(bf16)


def decode_body(
    len_ref, q_ref, dl_ref, dr_ref, nl_ref, nr_ref, wk_ref, wv_ref, out_ref, *, rows, scale
):
    heads, _, vdim = wv_ref.shape
    dec_rows, slots, latent = dl_ref.shape
    lat, rot = stacked_queries(q_ref[rows:, :], wk_ref)
    cache = dl_ref[...].reshape(dec_rows * slots, latent)
    cache_rot = dr_ref[...].reshape(dec_rows * slots, dr_ref.shape[2])
    new = nl_ref[rows:, :]
    old = (mm_t(lat, cache) + mm_t(rot, cache_rot)) * scale
    cur = (mm_t(lat, new) + mm_t(rot, nr_ref[rows:, :])) * scale
    row = lax.broadcasted_iota(jnp.int32, old.shape, 0) % tail
    column = lax.broadcasted_iota(jnp.int32, old.shape, 1)
    live = row < 0
    for b in range(dec_rows):
        live |= (row == b) & (column >= b * slots) & (column < b * slots + len_ref[b])
    old = jnp.where(live, old, masked)
    row = lax.broadcasted_iota(jnp.int32, cur.shape, 0) % tail
    cur = jnp.where(row == lax.broadcasted_iota(jnp.int32, cur.shape, 1), cur, masked)
    peak = jnp.maximum(
        jnp.max(old, axis=1, keepdims=True), jnp.max(cur, axis=1, keepdims=True)
    )
    w_old, w_cur = jnp.exp(old - peak), jnp.exp(cur - peak)
    total = jnp.sum(w_old, axis=1, keepdims=True) + jnp.sum(w_cur, axis=1, keepdims=True)
    mix = (mm(w_old.astype(bf16), cache) + mm(w_cur.astype(bf16), new)).astype(bf16)
    for h in range(heads):
        span = slice(h * tail, (h + 1) * tail)
        value = mm(mix[span], wv_ref[h]).astype(bf16).astype(f32)
        out_ref[:, h * vdim : (h + 1) * vdim] = (value / total[span]).astype(bf16)


def merge_body(*refs, rows, vdim):
    out_ref, dec_ref, parts = refs[-1], refs[-2], refs[:-2]
    width = out_ref.shape[1]
    levels = [
        jnp.sum(p[rows : rows + tail, :].astype(f32), axis=0, keepdims=True) for p in parts
    ]
    peak = functools.reduce(jnp.maximum, levels)
    shares = [jnp.exp(level - peak) for level in levels]
    total = functools.reduce(jnp.add, shares)
    for at in range(0, width, vdim):
        lanes = slice(at, at + vdim)
        acc = None
        for p, share in zip(parts, shares):
            factor = jnp.transpose(jnp.broadcast_to((share / total)[:, lanes], (vdim, vdim)))
            term = p[:rows, lanes].astype(f32) * factor
            acc = term if acc is None else acc + term
        out_ref[:rows, lanes] = acc.astype(bf16)
    out_ref[rows:, :] = dec_ref[...]


def output_body(*refs, rows):
    at_ref, parts, w_ref, piece_ref, dec_ref = refs[0], refs[1:-3], refs[-3], refs[-2], refs[-1]
    width = parts[0].shape[1]
    acc = None
    for k, p in enumerate(parts):
        first = pl.multiple_of(at_ref[k] * width, width)
        term = mm(p[...], w_ref[pl.ds(first, width), :])
        acc = term if acc is None else acc + term
    piece_ref[...] = acc[:rows].astype(bf16)
    dec_ref[...] = acc[rows : rows + dec_ref.shape[0]].astype(bf16)


def kernel_call(body, args, outs, flops, name, scalars=0, **static):
    vm = pl.BlockSpec(memory_space=pltpu.VMEM)
    sm = pl.BlockSpec(memory_space=pltpu.SMEM)
    nbytes = sum(a.size * a.dtype.itemsize for a in args)
    single = len(outs) == 1
    return pl.pallas_call(
        functools.partial(body, **static),
        in_specs=[sm] * scalars + [vm] * (len(args) - scalars),
        out_specs=vm if single else [vm] * len(outs),
        out_shape=outs[0] if single else list(outs),
        cost_estimate=pl.CostEstimate(flops=flops, bytes_accessed=nbytes, transcendentals=0),
        name=name,
    )(*args)


def flip(value, axis, k):
    count = lax.axis_size(axis)
    return lax.ppermute(value, axis, [(i, i ^ k) for i in range(count)])


def shards(
    piece_tokens,
    dec_tokens,
    norm_gain,
    w_query_nope,
    w_query_rope,
    w_latent,
    w_key_rope,
    latent_gain,
    w_key_up,
    w_value_up,
    w_out,
    prompt_latent,
    prompt_rope,
    dec_latent,
    dec_rope,
    dec_lengths,
):
    rows, model = piece_tokens.shape
    dec_rows, slots, latent = dec_latent.shape
    cached = prompt_latent.shape[0]
    heads, nope, _ = w_key_up.shape
    vdim = w_value_up.shape[2]
    rope = w_key_rope.shape[1]
    scale = (nope + rope) ** (-0.5)
    n_kv, n_tp = lax.axis_size("kv"), lax.axis_size("tp")
    me, lane = lax.axis_index("kv"), lax.axis_index("tp")
    padded = rows + tail
    shape = jax.ShapeDtypeStruct
    place = cached * n_kv + me * rows + jnp.arange(rows, dtype=jnp.int32)
    positions = jnp.concatenate(
        [place, dec_lengths, jnp.zeros((tail - dec_rows,), jnp.int32)]
    )
    table = tables(positions, rope)
    q_width = heads * (nope + rope)
    normed, query = kernel_call(
        query_body,
        (piece_tokens, dec_tokens, norm_gain[None], w_query_nope, w_query_rope, table),
        (shape((padded, model), bf16), shape((padded, q_width), bf16)),
        2 * padded * model * q_width,
        "query",
        half=rope // 2,
    )
    own = query[:rows]
    blocks = [own]
    for k in range(1, n_kv):
        low = k & -k
        blocks.append(flip(blocks[k ^ low], "kv", low))
    new_latent, new_rot = kernel_call(
        latent_body,
        (normed, latent_gain[None], w_latent, w_key_rope, table),
        (shape((padded, latent), bf16), shape((padded, rope), bf16)),
        2 * padded * model * (latent + rope),
        "latent",
        half=rope // 2,
    )
    keys = heads * rows * (cached + rows)
    parts = []
    for k in range(n_kv):
        offset = ((me ^ k) - me) * rows
        parts.append(
            kernel_call(
                attend_body,
                (
                    offset.astype(jnp.int32)[None],
                    blocks[k],
                    prompt_latent,
                    prompt_rope,
                    new_latent,
                    new_rot,
                    w_key_up,
                    w_value_up,
                ),
                (shape((padded, heads * vdim), bf16),),
                4 * keys * (latent + rope),
                "attend",
                scalars=1,
                rows=rows,
                scale=scale,
            )
        )
    parts = [parts[0]] + [flip(parts[k], "kv", k) for k in range(1, n_kv)]
    dec_attn = kernel_call(
        decode_body,
        (dec_lengths, query, dec_latent, dec_rope, new_latent, new_rot, w_key_up, w_value_up),
        (shape((tail, heads * vdim), bf16),),
        64 * heads * tail * dec_rows * slots * (latent + rope),
        "decode",
        scalars=1,
        rows=rows,
        scale=scale,
    )
    attended = kernel_call(
        merge_body,
        (*parts, dec_attn),
        (shape((padded, heads * vdim), bf16),),
        16 * rows * heads * vdim * n_kv,
        "merge",
        rows=rows,
        vdim=vdim,
    )
    gathered = {0: attended}
    for k in range(2, n_tp, 2):
        gathered[k] = flip(attended, "tp", k)
    for k in range(0, n_tp, 2):
        gathered[k + 1] = flip(gathered[k], "tp", 1)
    order = sorted(gathered)
    source = jnp.stack([lane ^ k for k in order]).astype(jnp.int32)
    return kernel_call(
        output_body,
        (source, *[gathered[k] for k in order], w_out),
        (shape((rows, w_out.shape[1]), bf16), shape((dec_rows, w_out.shape[1]), bf16)),
        2 * padded * w_out.shape[0] * w_out.shape[1],
        "output",
        scalars=1,
        rows=rows,
    )


def solution(mesh):
    in_specs = (
        P("kv", None),
        P("kv", None),
        P(),
        P(None, "tp"),
        P(None, "tp"),
        P(),
        P(),
        P(),
        P("tp", None, None),
        P("tp", None, None),
        P(None, "tp"),
        P("kv", None),
        P("kv", None),
        P("kv", None, None),
        P("kv", None, None),
        P("kv"),
    )
    out_specs = (P("kv", "tp"), P("kv", "tp"))

    def step(*args):
        return tuple(shards(*args))

    return jax.shard_map(step, mesh=mesh, in_specs=in_specs, out_specs=out_specs, check_vma=False)
```

```python
import functools

import jax
import jax.numpy as jnp
import numpy as np
from jax import lax
from jax.experimental import pallas as pl
from jax.experimental.pallas import tpu as pltpu
from jax.sharding import PartitionSpec as P

epsilon = 1e-06
rope_base = 10000.0
masked = -1e30
f32 = jnp.float32
bf16 = jnp.bfloat16
tail = 16


def mm(a, b):
    return jnp.dot(a, b, preferred_element_type=f32)


def mm_t(a, b):
    return lax.dot_general(a, b, (((1,), (1,)), ((), ())), preferred_element_type=f32)


def normalize(values, gain_row):
    mean_sq = jnp.mean(values * values, axis=-1, keepdims=True)
    return values * lax.rsqrt(mean_sq + epsilon) * gain_row


def rotate(values, cosines, sines, half):
    width = values.shape[1]
    lane = lax.broadcasted_iota(jnp.int32, values.shape, 1)
    front = (lane % (2 * half)) < half
    partner = jnp.where(front, pltpu.roll(values, width - half, 1), pltpu.roll(values, half, 1))
    return values * cosines + partner * jnp.where(front, -sines, sines)


def angle_tables(base_ref, len_ref, frequency, rows):
    row = lax.broadcasted_iota(jnp.int32, (rows + tail, frequency.shape[1]), 0)
    place = base_ref[0] + row
    for b in range(len_ref.shape[0]):
        place = jnp.where(row == rows + b, len_ref[b], place)
    angles = place.astype(f32) * frequency
    return jnp.cos(angles), jnp.sin(angles)


def normed_rows(piece, dec, gain):
    dec = normalize(dec.astype(f32), gain)
    dec = jnp.concatenate([dec, jnp.zeros((tail - dec.shape[0], dec.shape[1]), f32)], axis=0)
    piece = normalize(piece.astype(f32), gain)
    return jnp.concatenate([piece.astype(bf16), dec.astype(bf16)], axis=0)


def query_body(get, base_ref, len_ref, q_ref, dec_ref, *, half):
    piece = get(0)[...]
    rows = piece.shape[0]
    normed = normed_rows(piece, get(1)[...], get(2)[...])
    cosines, sines = angle_tables(base_ref, len_ref, get(3)[...], rows)
    raw = mm(normed, get(4)[...])
    nope = mm(normed, get(5)[...]).astype(bf16)
    first = nope.shape[1]
    q_ref[:, :first] = nope[:rows]
    dec_ref[:, :first] = nope[rows:]
    for at in range(0, raw.shape[1], 4 * half):
        lanes = slice(first + at, first + at + 4 * half)
        part = rotate(raw[:, at : at + 4 * half], cosines, sines, half).astype(bf16)
        q_ref[:, lanes] = part[:rows]
        dec_ref[:, lanes] = part[rows:]


def stacked_queries(q, wk_ref):
    heads, nope, _ = wk_ref.shape
    rope = (q.shape[1] - heads * nope) // heads
    lat = [mm(q[:, h * nope : (h + 1) * nope], wk_ref[h]).astype(bf16) for h in range(heads)]
    first = heads * nope
    rot = [q[:, first + h * rope : first + (h + 1) * rope] for h in range(heads)]
    return jnp.concatenate(lat, axis=0), jnp.concatenate(rot, axis=0)


def softmax_parts(old, cur):
    peak = jnp.maximum(
        jnp.max(old, axis=1, keepdims=True), jnp.max(cur, axis=1, keepdims=True)
    )
    w_old, w_cur = jnp.exp(old - peak), jnp.exp(cur - peak)
    total = jnp.sum(w_old, axis=1, keepdims=True) + jnp.sum(w_cur, axis=1, keepdims=True)
    return w_old.astype(bf16), w_cur.astype(bf16), peak, total


def attend_one(offset, q, prompt, prompt_rot, new, new_rot, wk_ref, wv_ref, out_ref, scale):
    rows = q.shape[0]
    heads, _, vdim = wv_ref.shape
    lat, rot = stacked_queries(q, wk_ref)
    old = (mm_t(lat, prompt) + mm(rot, prompt_rot)) * scale
    cur = (mm_t(lat, new) + mm_t(rot, new_rot)) * scale
    row = lax.broadcasted_iota(jnp.int32, cur.shape, 0) % rows
    column = lax.broadcasted_iota(jnp.int32, cur.shape, 1)
    cur = jnp.where(column - row <= offset, cur, masked)
    w_old, w_cur, peak, total = softmax_parts(old, cur)
    mix = (mm(w_old, prompt) + mm(w_cur, new)).astype(bf16)
    level = peak + jnp.log(total)
    for h in range(heads):
        span = slice(h * rows, (h + 1) * rows)
        lanes = slice(h * vdim, (h + 1) * vdim)
        value = mm(mix[span], wv_ref[h])
        out_ref[:rows, lanes] = (value / total[span]).astype(bf16)
        flat = jnp.transpose(jnp.broadcast_to(level[span], (rows, 128)))[:tail]
        high = flat.astype(bf16).astype(f32)
        middle = (flat - high).astype(bf16).astype(f32)
        low = flat - high - middle
        line = lax.broadcasted_iota(jnp.int32, flat.shape, 0)
        parts = jnp.where(line == 0, high, jnp.where(line == 1, middle, low))
        out_ref[rows:, lanes] = jnp.where(line < 3, parts, 0.0).astype(bf16)


def local_body(get, base_ref, len_ref, part_ref, dec_ref, lat_ref, rot_ref, *, half, scale):
    piece = get(0)[...]
    rows = piece.shape[0]
    normed = normed_rows(piece, get(1)[...], get(2)[...])
    cosines, sines = angle_tables(base_ref, len_ref, get(3)[...], rows)
    raw = mm_t(normed, get(4)[...])
    both = rotate(jnp.concatenate([raw, raw], axis=1), cosines, sines, half)
    new_rot = both[:, : 2 * half].astype(bf16)
    new = normalize(mm(normed, get(5)[...]), get(6)[...]).astype(bf16)
    lat_ref[...] = new[:rows]
    rot_ref[...] = new_rot[:rows]
    wk_ref, prompt_rot, prompt, wv_ref = get(7), get(9)[...], get(10)[...], get(11)
    attend_one(
        0, get(8)[...], prompt, prompt_rot, new[:rows], new_rot[:rows], wk_ref, wv_ref,
        part_ref, scale,
    )
    heads, _, vdim = wv_ref.shape
    lat, rot = stacked_queries(get(12)[...], wk_ref)
    rope_cache, cache_ref = get(13), get(14)
    dec_rows, slots, latent = cache_ref.shape
    cache = cache_ref[...].reshape(dec_rows * slots, latent)
    turned = jnp.concatenate([mm(rot, rope_cache[b]) for b in range(dec_rows)], axis=1)
    old = (mm_t(lat, cache) + turned) * scale
    cur = (mm_t(lat, new[rows:]) + mm_t(rot, new_rot[rows:])) * scale
    row = lax.broadcasted_iota(jnp.int32, old.shape, 0) % tail
    column = lax.broadcasted_iota(jnp.int32, old.shape, 1)
    live = row < 0
    for b in range(dec_rows):
        live |= (row == b) & (column >= b * slots) & (column < b * slots + len_ref[b])
    old = jnp.where(live, old, masked)
    row = lax.broadcasted_iota(jnp.int32, cur.shape, 0) % tail
    cur = jnp.where(row == lax.broadcasted_iota(jnp.int32, cur.shape, 1), cur, masked)
    w_old, w_cur, _, total = softmax_parts(old, cur)
    mix = (mm(w_old, cache) + mm(w_cur, new[rows:])).astype(bf16)
    for h in range(heads):
        span = slice(h * tail, (h + 1) * tail)
        value = mm(mix[span], wv_ref[h]).astype(bf16).astype(f32)
        dec_ref[:, h * vdim : (h + 1) * vdim] = (value / total[span]).astype(bf16)


def attend_body(get, me_ref, *outs, first, scale):
    wk_ref, prompt_rot, prompt, new_rot, new, wv_ref = [get(i) for i in range(6)]
    for i, out_ref in enumerate(outs):
        q = get(6 + i)[...]
        offset = ((me_ref[0] ^ (first + i)) - me_ref[0]) * q.shape[0]
        attend_one(
            offset, q, prompt[...], prompt_rot[...], new[...], new_rot[...], wk_ref, wv_ref,
            out_ref, scale,
        )


def merge_body(get, out_ref, *, rows, vdim, count):
    parts = [get(i) for i in range(count)]
    width = out_ref.shape[1]
    levels = [
        jnp.sum(p[rows : rows + tail, :].astype(f32), axis=0, keepdims=True) for p in parts
    ]
    peak = functools.reduce(jnp.maximum, levels)
    shares = [jnp.exp(level - peak) for level in levels]
    total = functools.reduce(jnp.add, shares)
    for at in range(0, width, vdim):
        lanes = slice(at, at + vdim)
        acc = None
        for p, share in zip(parts, shares):
            factor = jnp.transpose(jnp.broadcast_to((share / total)[:, lanes], (vdim, vdim)))
            term = p[:rows, lanes].astype(f32) * factor
            acc = term if acc is None else acc + term
        out_ref[:rows, lanes] = acc.astype(bf16)
    out_ref[rows:, :] = get(count)[...]


def output_body(get, at_ref, piece_ref, dec_ref, *, rows, order):
    w_ref = get(0)
    acc = None
    for i, k in enumerate(order):
        p = get(1 + i)[...]
        width = p.shape[1]
        first = pl.multiple_of((at_ref[0] ^ k) * width, width)
        term = mm(p, w_ref[pl.ds(first, width), :])
        acc = term if acc is None else acc + term
    piece_ref[...] = acc[:rows].astype(bf16)
    dec_ref[...] = acc[rows : rows + dec_ref.shape[0]].astype(bf16)


def kernel_call(body, scalars, args, outs, flops, name, **static):
    n_s, n_a, n_o = len(scalars), len(args), len(outs)

    def staged(*refs):
        given, rest = refs[:n_s], refs[n_s:]
        sources, results, slots, sems = rest[:n_a], rest[n_a : n_a + n_o], rest[n_a + n_o : -1], rest[-1]
        copies = [pltpu.make_async_copy(sources[i], slots[i], sems.at[i]) for i in range(n_a)]
        for copy in copies:
            copy.start()
        waited = set()

        def get(i):
            if i not in waited:
                copies[i].wait()
                waited.add(i)
            return slots[i]

        body(get, *given, *results, **static)

    vm = pl.BlockSpec(memory_space=pltpu.VMEM)
    sm = pl.BlockSpec(memory_space=pltpu.SMEM)
    anywhere = pl.BlockSpec(memory_space=pl.ANY)
    nbytes = sum(a.size * a.dtype.itemsize for a in args)
    single = n_o == 1
    return pl.pallas_call(
        staged,
        in_specs=[sm] * n_s + [anywhere] * n_a,
        out_specs=vm if single else [vm] * n_o,
        out_shape=outs[0] if single else list(outs),
        scratch_shapes=[pltpu.VMEM(a.shape, a.dtype) for a in args]
        + [pltpu.SemaphoreType.DMA((n_a,))],
        cost_estimate=pl.CostEstimate(flops=flops, bytes_accessed=nbytes, transcendentals=0),
        name=name,
    )(*scalars, *args)


def flip(value, axis, k):
    count = lax.axis_size(axis)
    return lax.ppermute(value, axis, [(i, i ^ k) for i in range(count)])


def shards(
    piece_tokens,
    dec_tokens,
    norm_gain,
    w_query_nope,
    w_query_rope,
    w_latent,
    w_key_rope,
    latent_gain,
    w_key_up,
    w_value_up,
    w_out,
    prompt_latent,
    prompt_rope,
    dec_latent,
    dec_rope,
    dec_lengths,
):
    rows, model = piece_tokens.shape
    dec_rows, slots, latent = dec_latent.shape
    cached = prompt_latent.shape[0]
    heads, nope, _ = w_key_up.shape
    vdim = w_value_up.shape[2]
    rope = w_key_rope.shape[1]
    scale = (nope + rope) ** (-0.5)
    n_kv, n_tp = lax.axis_size("kv"), lax.axis_size("tp")
    me, lane = lax.axis_index("kv"), lax.axis_index("tp")
    padded = rows + tail
    shape = jax.ShapeDtypeStruct
    half = rope // 2
    base = (cached * n_kv + me * rows).astype(jnp.int32)[None]
    frequency = np.tile(rope_base ** (-np.arange(half) / half), 4)[None].astype(np.float32)
    frequency = jnp.asarray(frequency)
    q_width = heads * (nope + rope)
    width = heads * vdim
    part = shape((padded, width), bf16)
    blocks, dec_query = kernel_call(
        query_body,
        (base, dec_lengths),
        (piece_tokens, dec_tokens, norm_gain[None], frequency, w_query_rope, w_query_nope),
        (shape((rows, q_width), bf16), shape((tail, q_width), bf16)),
        2 * padded * model * q_width,
        "query",
        half=half,
    )
    blocks = [blocks]
    for k in range(1, n_kv):
        low = k & -k
        blocks.append(flip(blocks[k ^ low], "kv", low))
    keys = heads * rows * (cached + rows)
    prompt_turned = prompt_rope.T
    own, dec_attn, new_latent, new_rot = kernel_call(
        local_body,
        (base, dec_lengths),
        (
            piece_tokens,
            dec_tokens,
            norm_gain[None],
            frequency,
            w_key_rope.T,
            w_latent,
            latent_gain[None],
            w_key_up,
            blocks[0],
            prompt_turned,
            prompt_latent,
            w_value_up,
            dec_query,
            jnp.swapaxes(dec_rope, 1, 2),
            dec_latent,
        ),
        (part, shape((tail, width), bf16), shape((rows, latent), bf16), shape((rows, rope), bf16)),
        8 * keys * (latent + rope),
        "local",
        half=half,
        scale=scale,
    )
    parts = [own]
    first = 1
    while first < n_kv:
        count = min(first, n_kv - first)
        group = kernel_call(
            attend_body,
            (me.astype(jnp.int32)[None],),
            (w_key_up, prompt_turned, prompt_latent, new_rot, new_latent, w_value_up)
            + tuple(blocks[first : first + count]),
            (part,) * count,
            4 * count * keys * (latent + rope),
            "attend",
            first=first,
            scale=scale,
        )
        group = [group] if count == 1 else group
        parts += [flip(value, "kv", first + i) for i, value in enumerate(group)]
        first += count
    attended = kernel_call(
        merge_body,
        (),
        (*parts, dec_attn),
        (part,),
        16 * rows * width * n_kv,
        "merge",
        rows=rows,
        vdim=vdim,
        count=n_kv,
    )
    gathered = {0: attended}
    for k in range(2, n_tp, 2):
        gathered[k] = flip(attended, "tp", k)
    for k in range(0, n_tp, 2):
        gathered[k + 1] = flip(gathered[k], "tp", 1)
    order = sorted(gathered)
    return kernel_call(
        output_body,
        (lane.astype(jnp.int32)[None],),
        (w_out, *[gathered[k] for k in order]),
        (shape((rows, w_out.shape[1]), bf16), shape((dec_rows, w_out.shape[1]), bf16)),
        2 * padded * w_out.shape[0] * w_out.shape[1],
        "output",
        rows=rows,
        order=tuple(order),
    )


def solution(mesh):
    in_specs = (
        P("kv", None),
        P("kv", None),
        P(),
        P(None, "tp"),
        P(None, "tp"),
        P(),
        P(),
        P(),
        P("tp", None, None),
        P("tp", None, None),
        P(None, "tp"),
        P("kv", None),
        P("kv", None),
        P("kv", None, None),
        P("kv", None, None),
        P("kv"),
    )
    out_specs = (P("kv", "tp"), P("kv", "tp"))

    def step(*args):
        return tuple(shards(*args))

    return jax.shard_map(step, mesh=mesh, in_specs=in_specs, out_specs=out_specs, check_vma=False)
```

```python
import functools

import jax
import jax.numpy as jnp
import numpy as np
from jax import lax
from jax.experimental import pallas as pl
from jax.experimental.pallas import tpu as pltpu
from jax.sharding import PartitionSpec as P


epsilon = 1e-06
rope_base = 10000.0
masked = -1e30
f32 = jnp.float32
bf16 = jnp.bfloat16
tail = 16


def mm(a, b):
    return jnp.dot(a, b, preferred_element_type=f32)


def mm_t(a, b):
    return lax.dot_general(a, b, (((1,), (1,)), ((), ())), preferred_element_type=f32)


def normalize(values, gain_row):
    mean_sq = jnp.mean(values * values, axis=-1, keepdims=True)
    return values * lax.rsqrt(mean_sq + epsilon) * gain_row


def rotate(values, cosines, sines, half):
    width = values.shape[1]
    lane = lax.broadcasted_iota(jnp.int32, values.shape, 1)
    front = (lane % (2 * half)) < half
    partner = jnp.where(front, pltpu.roll(values, width - half, 1), pltpu.roll(values, half, 1))
    return values * cosines + partner * jnp.where(front, -sines, sines)


def angle_tables(base_ref, len_ref, frequency, rows):
    row = lax.broadcasted_iota(jnp.int32, (rows + tail, frequency.shape[1]), 0)
    place = base_ref[0] + row
    for b in range(len_ref.shape[0]):
        place = jnp.where(row == rows + b, len_ref[b], place)
    angles = place.astype(f32) * frequency
    return jnp.cos(angles), jnp.sin(angles)


def normed_rows(piece, dec, gain):
    dec = normalize(dec.astype(f32), gain)
    dec = jnp.concatenate([dec, jnp.zeros((tail - dec.shape[0], dec.shape[1]), f32)], axis=0)
    piece = normalize(piece.astype(f32), gain)
    return jnp.concatenate([piece.astype(bf16), dec.astype(bf16)], axis=0)


def query_body(get, base_ref, len_ref, q_ref, dec_ref, *, half):
    piece = get(0)[...]
    rows = piece.shape[0]
    normed = normed_rows(piece, get(1)[...], get(2)[...])
    w_rope, w_nope = get(4), get(5)
    nope = mm(normed, w_nope[...]).astype(bf16)
    raw = mm(normed, w_rope[...])
    cosines, sines = angle_tables(base_ref, len_ref, get(3)[...], rows)
    first = nope.shape[1]
    q_ref[:, :first] = nope[:rows]
    dec_ref[:, :first] = nope[rows:]
    for at in range(0, raw.shape[1], 4 * half):
        lanes = slice(first + at, first + at + 4 * half)
        part = rotate(raw[:, at : at + 4 * half], cosines, sines, half).astype(bf16)
        q_ref[:, lanes] = part[:rows]
        dec_ref[:, lanes] = part[rows:]


def stacked_queries(q, wk_ref):
    heads, nope, _ = wk_ref.shape
    rope = (q.shape[1] - heads * nope) // heads
    lat = [mm(q[:, h * nope : (h + 1) * nope], wk_ref[h]).astype(bf16) for h in range(heads)]
    first = heads * nope
    rot = [q[:, first + h * rope : first + (h + 1) * rope] for h in range(heads)]
    return jnp.concatenate(lat, axis=0), jnp.concatenate(rot, axis=0)


def softmax_parts(old, cur):
    peak = jnp.maximum(
        jnp.max(old, axis=1, keepdims=True), jnp.max(cur, axis=1, keepdims=True)
    )
    w_old, w_cur = jnp.exp(old - peak), jnp.exp(cur - peak)
    total = jnp.sum(w_old, axis=1, keepdims=True) + jnp.sum(w_cur, axis=1, keepdims=True)
    return w_old.astype(bf16), w_cur.astype(bf16), peak, total


def attend_one(offset, q, prompt, prompt_rot, new, new_rot, wk_ref, wv_ref, out_ref, scale):
    rows = q.shape[0]
    heads, _, vdim = wv_ref.shape
    lat, rot = stacked_queries(q, wk_ref)
    old = (mm_t(lat, prompt) + mm(rot, prompt_rot)) * scale
    cur = (mm_t(lat, new) + mm_t(rot, new_rot)) * scale
    row = lax.broadcasted_iota(jnp.int32, cur.shape, 0) % rows
    column = lax.broadcasted_iota(jnp.int32, cur.shape, 1)
    cur = jnp.where(column - row <= offset, cur, masked)
    w_old, w_cur, peak, total = softmax_parts(old, cur)
    mix = (mm(w_old, prompt) + mm(w_cur, new)).astype(bf16)
    level = peak + jnp.log(total)
    for h in range(heads):
        span = slice(h * rows, (h + 1) * rows)
        lanes = slice(h * vdim, (h + 1) * vdim)
        value = mm(mix[span], wv_ref[h])
        out_ref[:rows, lanes] = (value / total[span]).astype(bf16)
        flat = jnp.transpose(jnp.broadcast_to(level[span], (rows, 128)))[:tail]
        high = flat.astype(bf16).astype(f32)
        middle = (flat - high).astype(bf16).astype(f32)
        low = flat - high - middle
        line = lax.broadcasted_iota(jnp.int32, flat.shape, 0)
        parts = jnp.where(line == 0, high, jnp.where(line == 1, middle, low))
        out_ref[rows:, lanes] = jnp.where(line < 3, parts, 0.0).astype(bf16)


def latent_body(get, base_ref, len_ref, lat_ref, rot_ref, *, half):
    piece = get(0)[...]
    rows = piece.shape[0]
    normed = normed_rows(piece, get(1)[...], get(2)[...])
    w_key, w_lat, gain = get(4), get(5), get(6)
    new = normalize(mm(normed, w_lat[...]), gain[...])
    raw = mm_t(normed, w_key[...])
    cosines, sines = angle_tables(base_ref, len_ref, get(3)[...], rows)
    both = rotate(jnp.concatenate([raw, raw], axis=1), cosines, sines, half)
    lat_ref[...] = new.astype(bf16)
    rot_ref[...] = both[:, : 2 * half].astype(bf16)


def decode_body(get, len_ref, dec_ref, *, rows, scale):
    wk_ref, q = get(0), get(1)[...]
    lat, rot = stacked_queries(q, wk_ref)
    new, new_rot = get(2)[rows:, :], get(3)[rows:, :]
    rope_cache, cache_ref, wv_ref = get(4), get(5), get(6)
    heads, _, vdim = wv_ref.shape
    dec_rows, slots, latent = cache_ref.shape
    cache = cache_ref[...].reshape(dec_rows * slots, latent)
    turned = jnp.concatenate([mm(rot, rope_cache[b]) for b in range(dec_rows)], axis=1)
    old = (mm_t(lat, cache) + turned) * scale
    cur = (mm_t(lat, new) + mm_t(rot, new_rot)) * scale
    row = lax.broadcasted_iota(jnp.int32, old.shape, 0) % tail
    column = lax.broadcasted_iota(jnp.int32, old.shape, 1)
    live = row < 0
    for b in range(dec_rows):
        live |= (row == b) & (column >= b * slots) & (column < b * slots + len_ref[b])
    old = jnp.where(live, old, masked)
    row = lax.broadcasted_iota(jnp.int32, cur.shape, 0) % tail
    cur = jnp.where(row == lax.broadcasted_iota(jnp.int32, cur.shape, 1), cur, masked)
    w_old, w_cur, _, total = softmax_parts(old, cur)
    mix = (mm(w_old, cache) + mm(w_cur, new)).astype(bf16)
    for h in range(heads):
        span = slice(h * tail, (h + 1) * tail)
        value = mm(mix[span], wv_ref[h]).astype(bf16).astype(f32)
        dec_ref[:, h * vdim : (h + 1) * vdim] = (value / total[span]).astype(bf16)


def attend_body(get, me_ref, *outs, first, scale):
    wk_ref, prompt_rot, prompt, new_rot, new, wv_ref = [get(i) for i in range(6)]
    for i, out_ref in enumerate(outs):
        q = get(6 + i)[...]
        offset = ((me_ref[0] ^ (first + i)) - me_ref[0]) * q.shape[0]
        attend_one(
            offset, q, prompt[...], prompt_rot[...], new[: q.shape[0], :],
            new_rot[: q.shape[0], :], wk_ref, wv_ref, out_ref, scale,
        )


def merge_body(get, out_ref, *, rows, vdim, count):
    parts = [get(i) for i in range(count)]
    width = out_ref.shape[1]
    levels = [
        jnp.sum(p[rows : rows + tail, :].astype(f32), axis=0, keepdims=True) for p in parts
    ]
    peak = functools.reduce(jnp.maximum, levels)
    shares = [jnp.exp(level - peak) for level in levels]
    total = functools.reduce(jnp.add, shares)
    for at in range(0, width, vdim):
        lanes = slice(at, at + vdim)
        acc = None
        for p, share in zip(parts, shares):
            factor = jnp.transpose(jnp.broadcast_to((share / total)[:, lanes], (vdim, vdim)))
            term = p[:rows, lanes].astype(f32) * factor
            acc = term if acc is None else acc + term
        out_ref[:rows, lanes] = acc.astype(bf16)
    out_ref[rows:, :] = get(count)[...]


def output_body(get, at_ref, piece_ref, dec_ref, *, rows, order):
    w_ref = get(0)
    acc = None
    for i, k in enumerate(order):
        p = get(1 + i)[...]
        width = p.shape[1]
        first = pl.multiple_of((at_ref[0] ^ k) * width, width)
        term = mm(p, w_ref[pl.ds(first, width), :])
        acc = term if acc is None else acc + term
    piece_ref[...] = acc[:rows].astype(bf16)
    dec_ref[...] = acc[rows : rows + dec_ref.shape[0]].astype(bf16)


def kernel_call(body, scalars, args, outs, flops, after=(), **static):
    n_s, n_a, n_o = len(scalars), len(args), len(outs)
    n_w = len(after)

    def staged(*refs):
        given, sources, rest = refs[:n_s], refs[n_s : n_s + n_a], refs[n_s + n_a + n_w :]
        results, slots, sems = rest[:n_o], rest[n_o:-1], rest[-1]
        copies = [pltpu.make_async_copy(sources[i], slots[i], sems.at[i]) for i in range(n_a)]
        for copy in copies:
            copy.start()
        waited = set()

        def get(i):
            if i not in waited:
                copies[i].wait()
                waited.add(i)
            return slots[i]

        body(get, *given, *results, **static)

    vm = pl.BlockSpec(memory_space=pltpu.VMEM)
    sm = pl.BlockSpec(memory_space=pltpu.SMEM)
    anywhere = pl.BlockSpec(memory_space=pl.ANY)
    nbytes = sum(a.size * a.dtype.itemsize for a in args)
    single = n_o == 1
    return pl.pallas_call(
        staged,
        in_specs=[sm] * n_s + [anywhere] * (n_a + n_w),
        out_specs=vm if single else [vm] * n_o,
        out_shape=outs[0] if single else list(outs),
        scratch_shapes=[pltpu.VMEM(a.shape, a.dtype) for a in args]
        + [pltpu.SemaphoreType.DMA((n_a,))],
        cost_estimate=pl.CostEstimate(flops=flops, bytes_accessed=nbytes, transcendentals=0),
    )(*scalars, *args, *after)


def flip(value, axis, k):
    count = lax.axis_size(axis)
    return lax.ppermute(value, axis, [(i, i ^ k) for i in range(count)])


def shards(
    piece_tokens,
    dec_tokens,
    norm_gain,
    w_query_nope,
    w_query_rope,
    w_latent,
    w_key_rope,
    latent_gain,
    w_key_up,
    w_value_up,
    w_out,
    prompt_latent,
    prompt_rope,
    dec_latent,
    dec_rope,
    dec_lengths,
):
    rows, model = piece_tokens.shape
    dec_rows, _, latent = dec_latent.shape
    cached = prompt_latent.shape[0]
    heads, nope, _ = w_key_up.shape
    vdim = w_value_up.shape[2]
    rope = w_key_rope.shape[1]
    scale = (nope + rope) ** (-0.5)
    n_kv, n_tp = lax.axis_size("kv"), lax.axis_size("tp")
    me, lane = lax.axis_index("kv"), lax.axis_index("tp")
    padded = rows + tail
    shape = jax.ShapeDtypeStruct
    half = rope // 2
    base = (cached * n_kv + me * rows).astype(jnp.int32)[None]
    frequency = np.tile(rope_base ** (-np.arange(half) / half), 4)[None].astype(np.float32)
    frequency = jnp.asarray(frequency)
    q_width = heads * (nope + rope)
    width = heads * vdim
    part = shape((padded, width), bf16)
    blocks, dec_query = kernel_call(
        query_body,
        (base, dec_lengths),
        (piece_tokens, dec_tokens, norm_gain[None], frequency, w_query_rope, w_query_nope),
        (shape((rows, q_width), bf16), shape((tail, q_width), bf16)),
        2 * padded * model * q_width,
        half=half,
    )
    keys = heads * rows * (cached + rows)
    blocks = [flip(blocks, "kv", k) for k in range(n_kv - 1, 0, -1)] + [blocks]
    blocks = blocks[::-1]
    prompt_turned = prompt_rope.T
    new_latent, new_rot = kernel_call(
        latent_body,
        (base, dec_lengths),
        (
            piece_tokens,
            dec_tokens,
            norm_gain[None],
            frequency,
            w_key_rope.T,
            w_latent,
            latent_gain[None],
        ),
        (shape((padded, latent), bf16), shape((padded, rope), bf16)),
        2 * padded * model * (latent + rope),
        half=half,
    )
    parts, last = [], ()
    first = 0
    while first < n_kv:
        count = min(2 if first == 0 else 1, n_kv - first)
        group = kernel_call(
            attend_body,
            (me.astype(jnp.int32)[None],),
            (w_key_up, prompt_turned, prompt_latent, new_rot, new_latent, w_value_up)
            + tuple(blocks[first : first + count]),
            (part,) * count,
            4 * count * keys * (latent + rope),
            after=last,
            first=first,
            scale=scale,
        )
        group = [group] if count == 1 else group
        last = (group[-1],)
        if first == 0:
            parts.append(group[0])
        if first + count > 1:
            parts.append(flip(group[-1], "kv", first + count - 1))
        first += count
    dec_attn = kernel_call(
        decode_body,
        (dec_lengths,),
        (
            w_key_up,
            dec_query,
            new_latent,
            new_rot,
            jnp.swapaxes(dec_rope, 1, 2),
            dec_latent,
            w_value_up,
        ),
        (shape((tail, width), bf16),),
        4 * keys * (latent + rope),
        after=last,
        rows=rows,
        scale=scale,
    )
    attended = kernel_call(
        merge_body,
        (),
        (*parts, dec_attn),
        (part,),
        16 * rows * width * n_kv,
        rows=rows,
        vdim=vdim,
        count=n_kv,
    )
    gathered = {0: attended}
    for k in range(2, n_tp, 2):
        gathered[k] = flip(attended, "tp", k)
    for k in range(0, n_tp, 2):
        gathered[k + 1] = flip(gathered[k], "tp", 1)
    order = sorted(gathered)
    return kernel_call(
        output_body,
        (lane.astype(jnp.int32)[None],),
        (w_out, *[gathered[k] for k in order]),
        (shape((rows, w_out.shape[1]), bf16), shape((dec_rows, w_out.shape[1]), bf16)),
        2 * padded * w_out.shape[0] * w_out.shape[1],
        rows=rows,
        order=tuple(order),
    )


def solution(mesh):
    in_specs = (
        P("kv", None),
        P("kv", None),
        P(),
        P(None, "tp"),
        P(None, "tp"),
        P(),
        P(),
        P(),
        P("tp", None, None),
        P("tp", None, None),
        P(None, "tp"),
        P("kv", None),
        P("kv", None),
        P("kv", None, None),
        P("kv", None, None),
        P("kv"),
    )
    out_specs = (P("kv", "tp"), P("kv", "tp"))

    def step(*args):
        return tuple(shards(*args))

    return jax.shard_map(
        step, mesh=mesh, in_specs=in_specs, out_specs=out_specs, check_vma=False
    )
```
